32 devices in a mesh: ep: 8 (over z, core), tp: 4 (over y, x).
Axes of the slice: x: 2, y: 2, z: 4, core: 2. Of those that a mesh axis runs over, the one named last changes fastest.
Arguments:
- mixer_value_input: bfloat16 [2048, 4096], P('ep', 'tp'), may hold values from -6 to 6
- input_state_matrix: bfloat16 [2048, 2048], P('ep', 'tp'), may hold values from -6 to 6
- output_state_matrix: bfloat16 [2048, 2048], P('ep', 'tp'), may hold values from -6 to 6
- output_gate_input: bfloat16 [2048, 4096], P('ep', 'tp'), may hold values from -6 to 6
- step_input: float32 [2048, 64], P('ep', 'tp'), may hold values from -6 to -2
- extra_log_decay: float32 [2048, 64], P('ep', 'tp'), may hold values from -1 to 0
- head_log_decay: float32 [64], P('tp'), may hold values from -10 to 1
- head_skip_scale: float32 [64], P('tp'), may hold values from 0.5 to 2
- value_kernel: float32 [4, 4096], P(None, 'tp'), may hold values from -3 to 3
- input_matrix_kernel: float32 [4, 2048], P(None, 'tp'), may hold values from -3 to 3
- output_matrix_kernel: float32 [4, 2048], P(None, 'tp'), may hold values from -3 to 3
- mixer_norm_scale: float32 [4096], P('tp'), may hold values from 0.1 to 1.9
- mixer_output_weight: bfloat16 [4096, 2048], P(None, 'tp'), may hold values from -0.09375 to 0.09375
- second_token_rows: bfloat16 [2048, 2048], P('ep'), may hold values from -6 to 6
- expert_norm_scale: float32 [2048], replicated, may hold values from 0.1 to 1.9
- routed_expert_index: int32 [2048, 4], P('ep'), may hold values from 0 to 15, all different within a row; in each aligned block of 256 rows (0 to 255, 256 to 511, ...) at most 96 rows name the same one
- routed_expert_weight: float32 [2048, 4], P('ep'), may hold values from 0.1 to 1
- routed_gate_weight: bfloat16 [16, 2048, 1024], P('ep', None, 'tp'), may hold values from -0.125 to 0.125
- routed_up_weight: bfloat16 [16, 2048, 1024], P('ep', None, 'tp'), may hold values from -0.125 to 0.125
- routed_down_weight: bfloat16 [16, 1024, 2048], P('ep', None, 'tp'), may hold values from -0.1875 to 0.1875
- shared_gate_weight: bfloat16 [2048, 1024], P(None, 'tp'), may hold values from -0.125 to 0.125
- shared_up_weight: bfloat16 [2048, 1024], P(None, 'tp'), may hold values from -0.125 to 0.125
- shared_down_weight: bfloat16 [1024, 2048], P(None, 'tp'), may hold values from -0.1875 to 0.1875
Outputs:
- mixer_output: bfloat16 [2048, 2048], P('ep', 'tp')
- routed_out: bfloat16 [2048, 2048], P('ep', 'tp')
The draws below stay inside these ranges and needn't reach their ends.
Inputs may be any that keep to these rules, and one draw needn't show every extreme that they name: `routed_expert_index`: in each aligned block of 256 rows (the rows of one index of ep) no expert is named more than 96 times, a bound that some block reaches.
All inputs are finite; a program needn't handle non-finite values.
Results may differ from the reference program's by a relative error of at most 0.012.
Values may be sent and summed in bfloat16 or wider, within the bound.
A program may use at most 64 MiB of HBM per device.

```python
import math
from functools import partial
import jax
import jax.numpy as jnp
import numpy as np
from jax import lax

D = 2048
HEADS = 64
HEAD_DIM = 64
INNER = 4096
GROUPS = 16
STATE = 128
CONV_TAPS = 4
BLOCK = 128
EXPERT_FF = 1024
SHARED_FF = 1024
EXPERTS = 16
TOP_K = 4
TOK_B = 256
TOKENS_A = 2048
TOKENS_B = 2048
CAP = 96
N_EP = 8


def draw_step_input(key, part):
    first_key, second_key = jax.random.split(jax.random.fold_in(key, 11))
    nblocks = TOKENS_A // BLOCK
    offset = jax.random.uniform(first_key, (nblocks, 1, HEADS), jnp.float32, -0.7, 0.7)
    noise = 0.3 * jax.random.truncated_normal(second_key, -2.0, 2.0, (nblocks, BLOCK, HEADS), jnp.float32)
    return (-4.0 + offset + noise).reshape(TOKENS_A, HEADS)


def draw_extra_log_decay(key, part):
    first_key, second_key = jax.random.split(jax.random.fold_in(key, 23))
    spots = jax.random.randint(first_key, (2,), 0, TOKENS_A)
    positions = jnp.arange(TOKENS_A)
    struck = jnp.any(positions[:, None] == spots[None, :], axis=1)
    losses = jnp.log(jax.random.uniform(second_key, (TOKENS_A, HEADS), jnp.float32, 0.5, 0.8))
    return jnp.where(struck[:, None], losses, 0.0).astype(jnp.float32)


def draw_head_log_decay(key, part):
    first_key, second_key, third_key = jax.random.split(jax.random.fold_in(key, 37), 3)
    slow_share = 0.5
    slow_heads = jax.random.uniform(first_key, (HEADS,), jnp.float32) < slow_share
    slow_rate = jax.random.uniform(second_key, (HEADS,), jnp.float32, 0.2, 1.0) * 30.0 / TOKENS_A
    fast_rate = jnp.exp(jax.random.uniform(third_key, (HEADS,), jnp.float32, jnp.log(0.5), jnp.log(1.5)))
    return jnp.log(jnp.where(slow_heads, slow_rate, fast_rate)).astype(jnp.float32)


def shard_levels(key, dims, shards, smallest, top_value):
    def one(axis_at, blocks):
        heights = jax.random.uniform(jax.random.fold_in(jax.random.fold_in(key, 6), axis_at), (blocks,), jnp.float32, smallest / len(shards), top_value / len(shards))
        return jnp.repeat(jnp.exp(heights), dims[axis_at] // blocks).reshape((-1,) + (1,) * (len(dims) - axis_at - 1))

    level = one(*shards[0])
    for cut in shards[1:]:
        level = level * one(*cut)
    return level


def deal_out(rng, own, number, rows, count, top, limit, lean):
    sequence = jax.random.permutation(rng, count)
    packed, common = portions_of(count, rows * top, limit, lean, True), portions_of(count, rows * top, limit, lean, False)
    places = jnp.arange(count)

    def named(tallies, turn):
        used = int((tallies > 0).sum())
        fixed = max(1, used // 4)
        moved = fixed + (places - fixed + turn * (used - fixed)) % max(1, count - fixed)
        return jnp.zeros((count,), jnp.int32).at[sequence[jnp.where(places < fixed, places, moved)]].set(jnp.asarray(tallies, jnp.int32))

    tallies = jnp.where(number % 4 == 0, named(packed, number // 4), named(common, number - number // 4 - 1))
    mixed = jax.random.permutation(jax.random.fold_in(own, 3), count)
    donor, sink = mixed[0:count // 2 * 2:2], mixed[1:count // 2 * 2:2]
    slack = jnp.minimum(tallies[donor] - 1, limit - tallies[sink]) // 2
    slack = jnp.where((donor == sequence[0]) | (sink == sequence[0]) | (tallies[sink] == 0), 0, jnp.maximum(slack, 0))
    moved = jax.random.randint(jax.random.fold_in(own, 4), (count // 2,), 0, 1 << 20) % (slack + 1)
    tallies = tallies.at[donor].add(-moved).at[sink].add(moved)
    labels = jnp.searchsorted(jnp.cumsum(tallies), jnp.arange(rows * top), side="right").astype(jnp.int32)
    table = labels.reshape(top, rows).T
    table = table[jax.random.permutation(jax.random.fold_in(own, 1), rows)]
    turn = jax.random.randint(jax.random.fold_in(own, 2), (rows, 1), 0, top)
    return jnp.take_along_axis(table, (jnp.arange(top)[None, :] + turn) % top, axis=1)


def portions_of(amount, total, bound, skew, full):
    weights = [(1 << 20) // math.isqrt(grade ** skew) + 1 for grade in range(1, amount + 1)]
    largest = bound if full else min(bound, max(-(-total // amount), total * weights[0] // sum(weights)))
    least = 1 if total - largest >= amount - 1 else 0
    counts, spare = [largest] + [least] * (amount - 1), total - largest - least * (amount - 1)
    while spare > 0:
        candidates = [i for i in range(1, amount) if counts[i] < largest] or [i for i in range(1, amount) if counts[i] < bound]
        whole, remaining = sum([weights[i] for i in candidates]), spare
        for i in candidates:
            extra = min(bound - counts[i], max(1, remaining * weights[i] // whole), spare)
            counts[i] = counts[i] + extra
            spare = spare - extra
    return np.array(counts)


def gaussian(key, shape, width, most, cuts=(), kind=jnp.bfloat16):
    array = jax.random.normal(key, shape, jnp.float32) * width
    if len(cuts) > 0:
        array = shard_levels(key, shape, cuts, -0.22, 0.18) * array
    return jnp.clip(array, min=-most, max=most).astype(kind)


def setup_inputs(seed: int = 0) -> dict:
    arg_keys = jax.random.split(jax.random.key(seed), 24)
    mixer_value_input = gaussian(arg_keys[0], (TOKENS_A, INNER), 1.0, 6.0, ((0, 8), (1, 4)))
    input_state_matrix = gaussian(arg_keys[1], (TOKENS_A, GROUPS * STATE), 1.0, 6.0, ((0, 8), (1, 4)))
    output_state_matrix = gaussian(arg_keys[2], (TOKENS_A, GROUPS * STATE), 1.0, 6.0, ((0, 8), (1, 4)))
    output_gate_input = gaussian(arg_keys[3], (TOKENS_A, INNER), 1.0, 6.0, ((0, 8), (1, 4)))
    step_input = draw_step_input(jax.random.fold_in(arg_keys[23], 71), 0)
    extra_log_decay = draw_extra_log_decay(jax.random.fold_in(arg_keys[23], 71), 0)
    head_log_decay = draw_head_log_decay(jax.random.fold_in(arg_keys[23], 71), 0)
    head_skip_scale = jnp.clip(0.5 + 1.5 * jax.random.uniform(arg_keys[7], (HEADS,), jnp.float32) ** shard_levels(arg_keys[7], (HEADS,), ((0, 4),), -0.2, 0.2), 0.5, 2.0)
    value_kernel = gaussian(arg_keys[8], (CONV_TAPS, INNER), 0.5, 3.0, ((1, 4),), jnp.float32)
    input_matrix_kernel = gaussian(arg_keys[9], (CONV_TAPS, GROUPS * STATE), 0.5, 3.0, ((1, 4),), jnp.float32)
    output_matrix_kernel = gaussian(arg_keys[10], (CONV_TAPS, GROUPS * STATE), 0.5, 3.0, ((1, 4),), jnp.float32)
    mixer_norm_scale = jnp.clip(1.0 + 0.18 * jax.random.normal(arg_keys[11], (INNER,), jnp.float32), 0.1, 1.9)
    mixer_output_weight = gaussian(arg_keys[12], (INNER, D), INNER ** -0.5, 0.09375, ((1, 4),))
    second_token_rows = gaussian(arg_keys[13], (TOKENS_B, D), 1.0, 6.0, ((0, 8),))
    expert_norm_scale = jnp.clip(1.0 + 0.18 * jax.random.normal(arg_keys[14], (D,), jnp.float32), 0.1, 1.9)
    routed_expert_index_keys = jax.random.split(jax.random.fold_in(arg_keys[15], 1), TOKENS_B // TOK_B)
    routed_expert_index_turns = jax.random.permutation(jax.random.fold_in(arg_keys[15], 3), TOKENS_B // TOK_B)
    routed_expert_index = jax.vmap(lambda own, number: deal_out(jax.random.fold_in(arg_keys[15], 2), own, number, TOK_B, EXPERTS, TOP_K, CAP, 2))(routed_expert_index_keys, routed_expert_index_turns).reshape((TOKENS_B, TOP_K))
    routed_expert_weight = jnp.clip(0.1 + 0.9 * jax.random.uniform(arg_keys[16], (TOKENS_B, TOP_K), jnp.float32) ** shard_levels(arg_keys[16], (TOKENS_B, TOP_K), ((0, 8),), -0.2, 0.2), 0.1, 1.0)
    routed_gate_weight = gaussian(arg_keys[17], (EXPERTS, D, EXPERT_FF), D ** -0.5, 0.125, ((0, 8), (2, 4)))
    routed_up_weight = gaussian(arg_keys[18], (EXPERTS, D, EXPERT_FF), D ** -0.5, 0.125, ((0, 8), (2, 4)))
    routed_down_weight = gaussian(arg_keys[19], (EXPERTS, EXPERT_FF, D), EXPERT_FF ** -0.5, 0.1875, ((0, 8), (2, 4)))
    shared_gate_weight = gaussian(arg_keys[20], (D, SHARED_FF), D ** -0.5, 0.125, ((1, 4),))
    shared_up_weight = gaussian(arg_keys[21], (D, SHARED_FF), D ** -0.5, 0.125, ((1, 4),))
    shared_down_weight = gaussian(arg_keys[22], (SHARED_FF, D), SHARED_FF ** -0.5, 0.1875, ((1, 4),))
    return {"mixer_value_input": mixer_value_input, "input_state_matrix": input_state_matrix, "output_state_matrix": output_state_matrix, "output_gate_input": output_gate_input, "step_input": step_input, "extra_log_decay": extra_log_decay, "head_log_decay": head_log_decay, "head_skip_scale": head_skip_scale, "value_kernel": value_kernel, "input_matrix_kernel": input_matrix_kernel, "output_matrix_kernel": output_matrix_kernel, "mixer_norm_scale": mixer_norm_scale, "mixer_output_weight": mixer_output_weight, "second_token_rows": second_token_rows, "expert_norm_scale": expert_norm_scale, "routed_expert_index": routed_expert_index, "routed_expert_weight": routed_expert_weight, "routed_gate_weight": routed_gate_weight, "routed_up_weight": routed_up_weight, "routed_down_weight": routed_down_weight, "shared_gate_weight": shared_gate_weight, "shared_up_weight": shared_up_weight, "shared_down_weight": shared_down_weight}


epsilon = 1e-05
precise = lax.Precision.HIGHEST

def conv_silu(source, weights):
    length = source.shape[0]
    padded = jnp.concatenate([jnp.zeros((CONV_TAPS - 1, source.shape[1]), source.dtype), source], axis=0)
    total_sum = jnp.zeros(source.shape, jnp.float32)
    for tap_index in range(CONV_TAPS):
        total_sum = total_sum + padded[tap_index:tap_index + length].astype(jnp.float32) * weights[tap_index]
    return jax.nn.silu(total_sum).astype(jnp.bfloat16)

def route_slots(route_block, experts, capacity):
    flat_ids = route_block.reshape(-1)
    onehot = (flat_ids[:, None] == jnp.arange(experts, dtype=jnp.int32)[None, :]).astype(jnp.int32)
    earlier = jnp.cumsum(onehot, axis=0) - onehot
    position_in = lax.optimization_barrier(jnp.sum(earlier * onehot, axis=1)).astype(jnp.int32)
    slot_index = (flat_ids * capacity + position_in).astype(jnp.int32)
    owner_row = (jnp.arange(flat_ids.shape[0], dtype=jnp.int32) // route_block.shape[1]).astype(jnp.int32)
    slot_owner = jnp.full((experts * capacity,), route_block.shape[0], jnp.int32).at[slot_index].set(owner_row)
    return (slot_owner, slot_index)

def spread_weights(slot_index, weights, count):
    return jnp.zeros((count,), jnp.float32).at[slot_index].set(weights)

def mixer_portion(mixer_value_input, input_state_matrix, output_state_matrix, output_gate_input, step_input, extra_log_decay, head_log_decay, head_skip_scale, value_kernel, input_matrix_kernel, output_matrix_kernel, mixer_norm_scale, mixer_output_weight):
    length = mixer_value_input.shape[0]
    values = conv_silu(mixer_value_input, value_kernel)
    in_mat = conv_silu(input_state_matrix, input_matrix_kernel)
    out_mat = conv_silu(output_state_matrix, output_matrix_kernel)
    step_length = jax.nn.softplus(step_input)
    decay_logarithm = -jnp.exp(head_log_decay)[None, :] * step_length + extra_log_decay
    head_ratio = HEADS // GROUPS
    nblocks = length // BLOCK
    value_wide = values.astype(jnp.float32).reshape(nblocks, BLOCK, HEADS, HEAD_DIM)
    in_wide = in_mat.astype(jnp.float32).reshape(nblocks, BLOCK, GROUPS, STATE)
    out_wide = out_mat.astype(jnp.float32).reshape(nblocks, BLOCK, GROUPS, STATE)
    step_blocks = step_length.reshape(nblocks, BLOCK, HEADS)
    log_blocks = decay_logarithm.reshape(nblocks, BLOCK, HEADS)
    lower_mask = jnp.tril(jnp.ones((BLOCK, BLOCK), bool))

    def advance(carried, inputs):
        value_blk, in_blk, out_blk, step_blk, log_blk = inputs
        running = jnp.cumsum(log_blk, axis=0)
        scaled = value_blk * step_blk[:, :, None]
        scores = jnp.einsum('ign,jgn->gij', out_blk, in_blk, precision=precise)
        scores = jnp.repeat(scores, head_ratio, axis=0)
        spread = jnp.transpose(running[:, None, :] - running[None, :, :], (2, 0, 1))
        decay_mat = jnp.where(lower_mask[None], jnp.exp(jnp.where(lower_mask[None], spread, 0.0)), 0.0)
        inside = jnp.einsum('hij,jhp->ihp', scores * decay_mat, scaled, precision=precise)
        out_head = jnp.repeat(out_blk, head_ratio, axis=1)
        in_head = jnp.repeat(in_blk, head_ratio, axis=1)
        carried_term = jnp.einsum('ihn,hpn->ihp', out_head, carried, precision=precise) * jnp.exp(running)[:, :, None]
        to_end = jnp.exp(running[-1][None, :] - running)
        updated = carried * jnp.exp(running[-1])[:, None, None] + jnp.einsum('jhn,jh,jhp->hpn', in_head, to_end, scaled, precision=precise)
        return (updated, inside + carried_term)
    start_state = jnp.zeros((HEADS, HEAD_DIM, STATE), jnp.float32)
    _, mixed_heads = lax.scan(advance, start_state, (value_wide, in_wide, out_wide, step_blocks, log_blocks))
    mixed_heads = mixed_heads.reshape(length, HEADS, HEAD_DIM) + head_skip_scale[None, :, None] * value_wide.reshape(length, HEADS, HEAD_DIM)
    gated_heads = mixed_heads * jax.nn.silu(output_gate_input.astype(jnp.float32)).reshape(length, HEADS, HEAD_DIM)
    grouped = gated_heads.reshape(length, GROUPS, head_ratio * HEAD_DIM)
    grouped = grouped * lax.rsqrt(lax.optimization_barrier(jnp.mean(grouped * grouped, axis=-1, keepdims=True)) + epsilon)
    normed = (grouped.reshape(length, HEADS * HEAD_DIM) * mixer_norm_scale).astype(jnp.bfloat16)
    return jnp.dot(normed, mixer_output_weight, preferred_element_type=jnp.float32).astype(jnp.bfloat16)

def expert_part(second_token_rows, expert_norm_scale, routed_expert_index, routed_expert_weight, routed_gate_weight, routed_up_weight, routed_down_weight, shared_gate_weight, shared_up_weight, shared_down_weight):
    total_rows = second_token_rows.shape[0]
    rows_wide = second_token_rows.astype(jnp.float32)
    normed = (rows_wide * lax.rsqrt(lax.optimization_barrier(jnp.mean(rows_wide * rows_wide, axis=-1, keepdims=True)) + epsilon) * expert_norm_scale).astype(jnp.bfloat16)
    block_ids = routed_expert_index.reshape(N_EP, TOK_B, TOP_K)
    tables, slot_sets = jax.vmap(partial(route_slots, experts=EXPERTS, capacity=CAP))(block_ids)
    offsets = (jnp.arange(N_EP, dtype=jnp.int32) * TOK_B)[:, None]
    global_rows = jnp.where(tables == TOK_B, total_rows, tables + offsets).astype(jnp.int32)
    slot_weights = jax.vmap(partial(spread_weights, count=EXPERTS * CAP))(slot_sets, routed_expert_weight.reshape(N_EP, TOK_B * TOP_K))
    expert_rows = global_rows.reshape(N_EP, EXPERTS, CAP).transpose(1, 0, 2).reshape(EXPERTS, N_EP * CAP)
    expert_weights = slot_weights.reshape(N_EP, EXPERTS, CAP).transpose(1, 0, 2).reshape(EXPERTS, N_EP * CAP)
    padded = jnp.concatenate([normed, jnp.zeros((1, normed.shape[1]), jnp.bfloat16)], axis=0)

    def one_expert(accumulated, inputs):
        row_index, weights, gate_w, up_w, down_w = inputs
        picked = jnp.take(padded, row_index, axis=0)
        hidden = (jax.nn.silu(jnp.dot(picked, gate_w, preferred_element_type=jnp.float32)) * jnp.dot(picked, up_w, preferred_element_type=jnp.float32)).astype(jnp.bfloat16)
        output = jnp.dot(hidden, down_w, preferred_element_type=jnp.float32).astype(jnp.bfloat16)
        return (accumulated.at[row_index].add(output.astype(jnp.float32) * weights[:, None]), None)
    accumulated = jnp.zeros((total_rows + 1, normed.shape[1]), jnp.float32)
    accumulated, _ = lax.scan(one_expert, accumulated, (expert_rows, expert_weights, routed_gate_weight, routed_up_weight, routed_down_weight))
    shared_hidden = (jax.nn.silu(jnp.dot(normed, shared_gate_weight, preferred_element_type=jnp.float32)) * jnp.dot(normed, shared_up_weight, preferred_element_type=jnp.float32)).astype(jnp.bfloat16)
    shared_result = jnp.dot(shared_hidden, shared_down_weight, preferred_element_type=jnp.float32)
    return (accumulated[:total_rows] + shared_result).astype(jnp.bfloat16)

def reference(mixer_value_input, input_state_matrix, output_state_matrix, output_gate_input, step_input, extra_log_decay, head_log_decay, head_skip_scale, value_kernel, input_matrix_kernel, output_matrix_kernel, mixer_norm_scale, mixer_output_weight, second_token_rows, expert_norm_scale, routed_expert_index, routed_expert_weight, routed_gate_weight, routed_up_weight, routed_down_weight, shared_gate_weight, shared_up_weight, shared_down_weight):
    mixer_output = mixer_portion(mixer_value_input, input_state_matrix, output_state_matrix, output_gate_input, step_input, extra_log_decay, head_log_decay, head_skip_scale, value_kernel, input_matrix_kernel, output_matrix_kernel, mixer_norm_scale, mixer_output_weight)
    routed_out = expert_part(second_token_rows, expert_norm_scale, routed_expert_index, routed_expert_weight, routed_gate_weight, routed_up_weight, routed_down_weight, shared_gate_weight, shared_up_weight, shared_down_weight)
    return (mixer_output, routed_out)
```

```python
import jax
import jax.numpy as jnp
from jax import lax
from jax.sharding import PartitionSpec as P

HEAD_DIM = 64
STATE = 128
CONV_TAPS = 4
BLOCK = 128
TOP_K = 4


epsilon = 1e-05
precise = lax.Precision.HIGHEST


def passed_along(x, axis, by):
    size = lax.axis_size(axis)
    pairs = [(i, i + by) for i in range(size) if 0 <= i + by < size]
    return lax.ppermute(x, axis, pairs)


def carried_in(total_log, state, axis):
    size = lax.axis_size(axis)
    place = lax.axis_index(axis)
    log = passed_along(total_log, axis, 1)
    hold = passed_along(state.astype(jnp.bfloat16), axis, 1).astype(jnp.float32)
    by = 1
    while by < size - 1:
        before = passed_along(hold.astype(jnp.bfloat16), axis, by).astype(jnp.float32)
        hold = hold + jnp.exp(log)[:, None, None] * before
        log = log + passed_along(log, axis, by)
        by *= 2
    return hold


def conv_silu(tail_rows, source, weights):
    length = source.shape[0]
    padded = jnp.concatenate([tail_rows, source], axis=0)
    total_sum = jnp.zeros(source.shape, jnp.float32)
    for tap_index in range(CONV_TAPS):
        total_sum = (
            total_sum
            + padded[tap_index : tap_index + length].astype(jnp.float32) * weights[tap_index]
        )
    return jax.nn.silu(total_sum).astype(jnp.bfloat16)


def carry_blocks(carried, inputs):
    block_decay, block_state = inputs
    return (carried * block_decay[:, None, None] + block_state, carried)


def earlier_counts(mask, rows):
    at = jnp.arange(rows)
    tri = (at[:, None] < at[None, :]).astype(jnp.bfloat16)
    return lax.dot_general(
        mask.astype(jnp.bfloat16),
        tri,
        (((mask.ndim - 1,), (0,)), ((), ())),
        preferred_element_type=jnp.float32,
    )


def on_device(
    mixer_value_input,
    input_state_matrix,
    output_state_matrix,
    output_gate_input,
    step_input,
    extra_log_decay,
    head_log_decay,
    head_skip_scale,
    value_kernel,
    input_matrix_kernel,
    output_matrix_kernel,
    mixer_norm_scale,
    mixer_output_weight,
    second_token_rows,
    expert_norm_scale,
    routed_expert_index,
    routed_expert_weight,
    routed_gate_weight,
    routed_up_weight,
    routed_down_weight,
    shared_gate_weight,
    shared_up_weight,
    shared_down_weight,
):
    length = mixer_value_input.shape[0]
    heads_local = step_input.shape[1]
    width_x = mixer_value_input.shape[1]
    width_b = input_state_matrix.shape[1]
    groups_local = width_b // STATE
    head_ratio = heads_local // groups_local
    nblocks = length // BLOCK
    lead_row = length - CONV_TAPS + 1
    edge_rows = jnp.concatenate(
        [
            mixer_value_input[lead_row:],
            input_state_matrix[lead_row:],
            output_state_matrix[lead_row:],
        ],
        axis=1,
    )
    tail_rows = passed_along(edge_rows, "ep", 1)
    rows_local = second_token_rows.shape[0]
    model_width = second_token_rows.shape[1]
    local_experts = routed_gate_weight.shape[0]
    ep_count = lax.axis_size("ep")
    experts = local_experts * ep_count
    capacity = max(2, 3 * rows_local * TOP_K // (2 * experts))
    col_width = model_width // lax.axis_size("tp")
    rows_wide = second_token_rows.astype(jnp.float32)
    normed = (
        rows_wide
        * lax.rsqrt(jnp.mean(rows_wide * rows_wide, axis=-1, keepdims=True) + epsilon)
        * expert_norm_scale
    ).astype(jnp.bfloat16)
    ids = routed_expert_index.T.astype(jnp.float32)
    id_rows = -(-ids.size // col_width)
    id_block = jnp.pad(
        ids.astype(jnp.bfloat16).reshape(-1), (0, id_rows * col_width - ids.size)
    ).reshape(id_rows, col_width)
    id_block = jnp.pad(id_block, ((0, -id_rows % 8), (0, 0)))
    my_columns = lax.dynamic_slice_in_dim(normed, lax.axis_index("tp") * col_width, col_width, 1)
    outgoing, value_rows, in_rows, out_rows = lax.optimization_barrier(
        (
            jnp.concatenate([my_columns, id_block], axis=0),
            mixer_value_input,
            input_state_matrix,
            output_state_matrix,
        )
    )
    everyone = lax.all_gather(outgoing, "ep", axis=0)
    values = conv_silu(tail_rows[:, :width_x], value_rows, value_kernel)
    in_mat = conv_silu(
        tail_rows[:, width_x : width_x + width_b], in_rows, input_matrix_kernel
    )
    out_mat = conv_silu(
        tail_rows[:, width_x + width_b :], out_rows, output_matrix_kernel
    )
    step_length = jax.nn.softplus(step_input)
    decay_logarithm = -jnp.exp(head_log_decay)[None, :] * step_length + extra_log_decay
    running = jnp.cumsum(decay_logarithm.reshape(nblocks, BLOCK, heads_local), axis=1)
    value_wide = values.astype(jnp.float32).reshape(nblocks, BLOCK, heads_local, HEAD_DIM)
    scaled = value_wide * step_length.reshape(nblocks, BLOCK, heads_local)[..., None]
    in_blocks = in_mat.reshape(nblocks, BLOCK, groups_local, STATE)
    out_blocks = out_mat.reshape(nblocks, BLOCK, groups_local, STATE)
    scores = jnp.einsum(
        "bign,bjgn->bgij", out_blocks, in_blocks, preferred_element_type=jnp.float32
    )
    scores = jnp.repeat(scores, head_ratio, axis=1)
    spread = jnp.transpose(running[:, :, None, :] - running[:, None, :, :], (0, 3, 1, 2))
    lower_mask = jnp.tril(jnp.ones((BLOCK, BLOCK), bool))[None, None]
    decay_mat = jnp.where(lower_mask, jnp.exp(jnp.where(lower_mask, spread, 0.0)), 0.0)
    inside = jnp.einsum("bhij,bjhp->bihp", scores * decay_mat, scaled, precision=precise)
    out_head = jnp.repeat(out_blocks.astype(jnp.float32), head_ratio, axis=2)
    in_head = jnp.repeat(in_blocks.astype(jnp.float32), head_ratio, axis=2)
    block_logs = running[:, -1]
    to_end = jnp.exp(block_logs[:, None, :] - running)
    block_state = jnp.einsum("bjhn,bjh,bjhp->bhpn", in_head, to_end, scaled, precision=precise)
    start_state = jnp.zeros((heads_local, HEAD_DIM, STATE), jnp.float32)
    local_total, local_prev = lax.scan(
        carry_blocks, start_state, (jnp.exp(block_logs), block_state)
    )
    before_logs = jnp.cumsum(block_logs, axis=0) - block_logs
    everyone, local_total = lax.optimization_barrier((everyone, local_total))
    incoming = carried_in(jnp.sum(block_logs, axis=0), local_total, "ep")
    their_rows = everyone[:, :rows_local]
    their_ids = everyone[:, rows_local : rows_local + id_rows].reshape(ep_count, -1)
    their_ids = their_ids[:, : ids.size].reshape(ep_count, TOP_K, rows_local).astype(jnp.float32)
    mine = (lax.axis_index("ep") * local_experts + jnp.arange(local_experts)).astype(jnp.float32)
    named = jnp.any(their_ids[:, None] == mine[None, :, None, None], axis=2)
    seat = jnp.where(named, earlier_counts(named, rows_local), -1.0)
    seats = jnp.arange(capacity, dtype=jnp.float32)
    pick = (seat[:, :, None, :] == seats[None, None, :, None]).astype(jnp.bfloat16)
    arrived = jnp.stack(
        [
            jnp.einsum(
                "bsr,brd->bsd", pick[:, j], their_rows, preferred_element_type=jnp.float32
            )
            .astype(jnp.bfloat16)
            .reshape(ep_count * capacity, col_width)
            for j in range(local_experts)
        ]
    )
    column_piece = lax.all_gather(arrived, "tp", axis=2, tiled=True)
    column_piece, incoming = lax.optimization_barrier((column_piece, incoming))
    entering = local_prev + jnp.exp(before_logs)[:, :, None, None] * incoming[None]
    carried_term = (
        jnp.einsum("bihn,bhpn->bihp", out_head, entering, precision=precise)
        * jnp.exp(running)[..., None]
    )
    mixed_heads = (inside + carried_term).reshape(length, heads_local, HEAD_DIM)
    mixed_heads = mixed_heads + head_skip_scale[None, :, None] * value_wide.reshape(
        length, heads_local, HEAD_DIM
    )
    gated_heads = mixed_heads * jax.nn.silu(output_gate_input.astype(jnp.float32)).reshape(
        length, heads_local, HEAD_DIM
    )
    grouped = gated_heads.reshape(length, groups_local, head_ratio * HEAD_DIM)
    grouped = grouped * lax.rsqrt(jnp.mean(grouped * grouped, axis=-1, keepdims=True) + epsilon)
    mixer_normed = (grouped.reshape(length, width_x) * mixer_norm_scale).astype(jnp.bfloat16)
    gate_pre = jnp.einsum(
        "esd,edf->esf", column_piece, routed_gate_weight, preferred_element_type=jnp.float32
    )
    up_pre = jnp.einsum(
        "esd,edf->esf", column_piece, routed_up_weight, preferred_element_type=jnp.float32
    )
    hidden = (jax.nn.silu(gate_pre) * up_pre).astype(jnp.bfloat16)
    shared_hidden = (
        jax.nn.silu(jnp.dot(normed, shared_gate_weight, preferred_element_type=jnp.float32))
        * jnp.dot(normed, shared_up_weight, preferred_element_type=jnp.float32)
    ).astype(jnp.bfloat16)
    slots = ep_count * capacity
    hidden_rows = jnp.concatenate(
        [hidden.reshape(local_experts * slots, hidden.shape[2]), shared_hidden], axis=0
    )
    whole_rows = lax.all_gather(hidden_rows, "tp", axis=1, tiled=True)
    whole_hidden = whole_rows[: local_experts * slots].reshape(local_experts, slots, -1)
    whole_shared = whole_rows[local_experts * slots :]
    whole_mix = lax.all_gather(mixer_normed, "tp", axis=1, tiled=True)
    mixer_output = jnp.dot(
        whole_mix, mixer_output_weight, preferred_element_type=jnp.float32
    ).astype(jnp.bfloat16)
    expert_result = jnp.einsum(
        "esf,efd->esd", whole_hidden, routed_down_weight, preferred_element_type=jnp.float32
    ).astype(jnp.bfloat16)
    going = jnp.concatenate(
        [expert_result[j].reshape(ep_count, capacity, col_width) for j in range(local_experts)],
        axis=1,
    )
    returned = lax.all_to_all(going, "ep", split_axis=0, concat_axis=0, tiled=True)
    returned = returned.reshape(experts * capacity, col_width)
    kinds = jnp.arange(experts, dtype=jnp.float32)
    chosen = ids[:, None, :] == kinds[None, :, None]
    count = earlier_counts(jnp.any(chosen, axis=0), rows_local)
    position = jnp.sum(jnp.where(chosen, count[None], 0.0), axis=1)
    slot = (ids * capacity + position).T.astype(jnp.int32)
    columns = jnp.arange(experts * capacity, dtype=jnp.int32)[None, :]
    spread = jnp.zeros((rows_local, experts * capacity), jnp.float32)
    for k in range(TOP_K):
        spread = spread + jnp.where(
            slot[:, k : k + 1] == columns, routed_expert_weight[:, k : k + 1], 0.0
        )
    high = lax.reduce_precision(spread, 8, 7)
    low = (spread - high).astype(jnp.bfloat16)
    routed_sum = jnp.dot(
        high.astype(jnp.bfloat16), returned, preferred_element_type=jnp.float32
    ) + jnp.dot(low, returned, preferred_element_type=jnp.float32)
    shared_result = jnp.dot(whole_shared, shared_down_weight, preferred_element_type=jnp.float32)
    routed_out = (routed_sum + shared_result).astype(jnp.bfloat16)
    return (mixer_output, routed_out)


def solution(mesh):
    return jax.shard_map(
        on_device,
        mesh=mesh,
        in_specs=(
            P("ep", "tp"),
            P("ep", "tp"),
            P("ep", "tp"),
            P("ep", "tp"),
            P("ep", "tp"),
            P("ep", "tp"),
            P("tp"),
            P("tp"),
            P(None, "tp"),
            P(None, "tp"),
            P(None, "tp"),
            P("tp"),
            P(None, "tp"),
            P("ep", None),
            P(),
            P("ep", None),
            P("ep", None),
            P("ep", None, "tp"),
            P("ep", None, "tp"),
            P("ep", None, "tp"),
            P(None, "tp"),
            P(None, "tp"),
            P(None, "tp"),
        ),
        out_specs=(P("ep", "tp"), P("ep", "tp")),
        check_vma=False,
    )
```

```python
import jax
import jax.numpy as jnp
from jax import lax
from jax.sharding import PartitionSpec as P

HEAD_DIM = 64
STATE = 128
CONV_TAPS = 4
BLOCK = 128
TOP_K = 4


epsilon = 1e-05
precise = lax.Precision.HIGHEST


def passed_along(x, axis, by):
    size = lax.axis_size(axis)
    pairs = [(i, i + by) for i in range(size) if 0 <= i + by < size]
    return lax.ppermute(x, axis, pairs)


def carried_in(total_log, state, axis):
    size = lax.axis_size(axis)
    place = lax.axis_index(axis)
    log = passed_along(total_log, axis, 1)
    hold = passed_along(state.astype(jnp.bfloat16), axis, 1).astype(jnp.float32)
    by = 1
    while by < size - 1:
        before = passed_along(hold.astype(jnp.bfloat16), axis, by).astype(jnp.float32)
        hold = hold + jnp.exp(log)[:, None, None] * before
        log = log + passed_along(log, axis, by)
        by *= 2
    return hold


def conv_silu(tail_rows, source, weights):
    length = source.shape[0]
    padded = jnp.concatenate([tail_rows, source], axis=0)
    total_sum = jnp.zeros(source.shape, jnp.float32)
    for tap_index in range(CONV_TAPS):
        total_sum = (
            total_sum
            + padded[tap_index : tap_index + length].astype(jnp.float32) * weights[tap_index]
        )
    return jax.nn.silu(total_sum).astype(jnp.bfloat16)


def carry_blocks(carried, inputs):
    block_decay, block_state = inputs
    return (carried * block_decay[:, None, None] + block_state, carried)


def earlier_counts(mask, rows):
    at = jnp.arange(rows)
    tri = (at[:, None] < at[None, :]).astype(jnp.bfloat16)
    return lax.dot_general(
        mask.astype(jnp.bfloat16),
        tri,
        (((mask.ndim - 1,), (0,)), ((), ())),
        preferred_element_type=jnp.float32,
    )


def on_device(
    mixer_value_input,
    input_state_matrix,
    output_state_matrix,
    output_gate_input,
    step_input,
    extra_log_decay,
    head_log_decay,
    head_skip_scale,
    value_kernel,
    input_matrix_kernel,
    output_matrix_kernel,
    mixer_norm_scale,
    mixer_output_weight,
    second_token_rows,
    expert_norm_scale,
    routed_expert_index,
    routed_expert_weight,
    routed_gate_weight,
    routed_up_weight,
    routed_down_weight,
    shared_gate_weight,
    shared_up_weight,
    shared_down_weight,
):
    length = mixer_value_input.shape[0]
    heads_local = step_input.shape[1]
    width_x = mixer_value_input.shape[1]
    width_b = input_state_matrix.shape[1]
    groups_local = width_b // STATE
    head_ratio = heads_local // groups_local
    nblocks = length // BLOCK
    lead_row = length - CONV_TAPS + 1
    edge_rows = jnp.concatenate(
        [
            mixer_value_input[lead_row:],
            input_state_matrix[lead_row:],
            output_state_matrix[lead_row:],
        ],
        axis=1,
    )
    tail_rows = passed_along(edge_rows, "ep", 1)
    rows_local = second_token_rows.shape[0]
    model_width = second_token_rows.shape[1]
    local_experts = routed_gate_weight.shape[0]
    ep_count = lax.axis_size("ep")
    experts = local_experts * ep_count
    capacity = max(2, 3 * rows_local * TOP_K // (2 * experts))
    col_width = model_width // lax.axis_size("tp")
    rows_wide = second_token_rows.astype(jnp.float32)
    normed = (
        rows_wide
        * lax.rsqrt(jnp.mean(rows_wide * rows_wide, axis=-1, keepdims=True) + epsilon)
        * expert_norm_scale
    ).astype(jnp.bfloat16)
    ids = routed_expert_index.T.astype(jnp.float32)
    id_rows = -(-ids.size // col_width)
    id_block = jnp.pad(
        ids.astype(jnp.bfloat16).reshape(-1), (0, id_rows * col_width - ids.size)
    ).reshape(id_rows, col_width)
    id_block = jnp.pad(id_block, ((0, -id_rows % 8), (0, 0)))
    my_columns = lax.dynamic_slice_in_dim(normed, lax.axis_index("tp") * col_width, col_width, 1)
    outgoing, value_rows, in_rows, out_rows = lax.optimization_barrier(
        (
            jnp.concatenate([my_columns, id_block], axis=0),
            mixer_value_input,
            input_state_matrix,
            output_state_matrix,
        )
    )
    everyone = lax.all_gather(outgoing, "ep", axis=0)
    values = conv_silu(tail_rows[:, :width_x], value_rows, value_kernel)
    in_mat = conv_silu(
        tail_rows[:, width_x : width_x + width_b], in_rows, input_matrix_kernel
    )
    out_mat = conv_silu(
        tail_rows[:, width_x + width_b :], out_rows, output_matrix_kernel
    )
    step_length = jax.nn.softplus(step_input)
    decay_logarithm = -jnp.exp(head_log_decay)[None, :] * step_length + extra_log_decay
    running = jnp.cumsum(decay_logarithm.reshape(nblocks, BLOCK, heads_local), axis=1)
    value_wide = values.astype(jnp.float32).reshape(nblocks, BLOCK, heads_local, HEAD_DIM)
    scaled = value_wide * step_length.reshape(nblocks, BLOCK, heads_local)[..., None]
    in_blocks = in_mat.reshape(nblocks, BLOCK, groups_local, STATE)
    out_blocks = out_mat.reshape(nblocks, BLOCK, groups_local, STATE)
    scores = jnp.einsum(
        "bign,bjgn->bgij", out_blocks, in_blocks, preferred_element_type=jnp.float32
    )
    scores = jnp.repeat(scores, head_ratio, axis=1)
    spread = jnp.transpose(running[:, :, None, :] - running[:, None, :, :], (0, 3, 1, 2))
    lower_mask = jnp.tril(jnp.ones((BLOCK, BLOCK), bool))[None, None]
    decay_mat = jnp.where(lower_mask, jnp.exp(jnp.where(lower_mask, spread, 0.0)), 0.0)
    inside = jnp.einsum("bhij,bjhp->bihp", scores * decay_mat, scaled, precision=precise)
    out_head = jnp.repeat(out_blocks.astype(jnp.float32), head_ratio, axis=2)
    in_head = jnp.repeat(in_blocks.astype(jnp.float32), head_ratio, axis=2)
    block_logs = running[:, -1]
    to_end = jnp.exp(block_logs[:, None, :] - running)
    block_state = jnp.einsum("bjhn,bjh,bjhp->bhpn", in_head, to_end, scaled, precision=precise)
    start_state = jnp.zeros((heads_local, HEAD_DIM, STATE), jnp.float32)
    local_total, local_prev = lax.scan(
        carry_blocks, start_state, (jnp.exp(block_logs), block_state)
    )
    before_logs = jnp.cumsum(block_logs, axis=0) - block_logs
    everyone, local_total = lax.optimization_barrier((everyone, local_total))
    incoming = carried_in(jnp.sum(block_logs, axis=0), local_total, "ep")
    their_rows = everyone[:, :rows_local]
    their_ids = everyone[:, rows_local : rows_local + id_rows].reshape(ep_count, -1)
    their_ids = their_ids[:, : ids.size].reshape(ep_count, TOP_K, rows_local).astype(jnp.float32)
    mine = (lax.axis_index("ep") * local_experts + jnp.arange(local_experts)).astype(jnp.float32)
    named = jnp.any(their_ids[:, None] == mine[None, :, None, None], axis=2)
    seat = jnp.where(named, earlier_counts(named, rows_local), -1.0)
    seats = jnp.arange(capacity, dtype=jnp.float32)
    pick = (seat[:, :, None, :] == seats[None, None, :, None]).astype(jnp.bfloat16)
    arrived = jnp.stack(
        [
            jnp.einsum(
                "bsr,brd->bsd", pick[:, j], their_rows, preferred_element_type=jnp.float32
            )
            .astype(jnp.bfloat16)
            .reshape(ep_count * capacity, col_width)
            for j in range(local_experts)
        ]
    )
    column_piece = lax.all_gather(arrived, "tp", axis=2, tiled=True)
    column_piece, incoming = lax.optimization_barrier((column_piece, incoming))
    entering = local_prev + jnp.exp(before_logs)[:, :, None, None] * incoming[None]
    carried_term = (
        jnp.einsum("bihn,bhpn->bihp", out_head, entering, precision=precise)
        * jnp.exp(running)[..., None]
    )
    mixed_heads = (inside + carried_term).reshape(length, heads_local, HEAD_DIM)
    mixed_heads = mixed_heads + head_skip_scale[None, :, None] * value_wide.reshape(
        length, heads_local, HEAD_DIM
    )
    gated_heads = mixed_heads * jax.nn.silu(output_gate_input.astype(jnp.float32)).reshape(
        length, heads_local, HEAD_DIM
    )
    grouped = gated_heads.reshape(length, groups_local, head_ratio * HEAD_DIM)
    grouped = grouped * lax.rsqrt(jnp.mean(grouped * grouped, axis=-1, keepdims=True) + epsilon)
    mixer_normed = (grouped.reshape(length, width_x) * mixer_norm_scale).astype(jnp.bfloat16)
    gate_pre = jnp.einsum(
        "esd,edf->esf", column_piece, routed_gate_weight, preferred_element_type=jnp.float32
    )
    up_pre = jnp.einsum(
        "esd,edf->esf", column_piece, routed_up_weight, preferred_element_type=jnp.float32
    )
    hidden = (jax.nn.silu(gate_pre) * up_pre).astype(jnp.bfloat16)
    shared_hidden = (
        jax.nn.silu(jnp.dot(normed, shared_gate_weight, preferred_element_type=jnp.float32))
        * jnp.dot(normed, shared_up_weight, preferred_element_type=jnp.float32)
    ).astype(jnp.bfloat16)
    whole_hidden = lax.all_gather(hidden, "tp", axis=2, tiled=True)
    both = lax.all_gather(
        jnp.concatenate([mixer_normed, shared_hidden], axis=1), "tp", axis=1, tiled=True
    ).reshape(length, lax.axis_size("tp"), -1)
    whole_mix = both[:, :, :width_x].reshape(length, -1)
    whole_shared = both[:, :, width_x:].reshape(length, -1)
    mixer_output = jnp.dot(
        whole_mix, mixer_output_weight, preferred_element_type=jnp.float32
    ).astype(jnp.bfloat16)
    expert_result = jnp.einsum(
        "esf,efd->esd", whole_hidden, routed_down_weight, preferred_element_type=jnp.float32
    ).astype(jnp.bfloat16)
    going = jnp.concatenate(
        [expert_result[j].reshape(ep_count, capacity, col_width) for j in range(local_experts)],
        axis=1,
    )
    returned = lax.all_to_all(going, "ep", split_axis=0, concat_axis=0, tiled=True)
    returned = returned.reshape(experts * capacity, col_width)
    kinds = jnp.arange(experts, dtype=jnp.float32)
    chosen = ids[:, None, :] == kinds[None, :, None]
    count = earlier_counts(jnp.any(chosen, axis=0), rows_local)
    position = jnp.sum(jnp.where(chosen, count[None], 0.0), axis=1)
    slot = (ids * capacity + position).T.astype(jnp.int32)
    columns = jnp.arange(experts * capacity, dtype=jnp.int32)[None, :]
    spread = jnp.zeros((rows_local, experts * capacity), jnp.float32)
    for k in range(TOP_K):
        spread = spread + jnp.where(
            slot[:, k : k + 1] == columns, routed_expert_weight[:, k : k + 1], 0.0
        )
    high = lax.reduce_precision(spread, 8, 7)
    low = (spread - high).astype(jnp.bfloat16)
    routed_sum = jnp.dot(
        high.astype(jnp.bfloat16), returned, preferred_element_type=jnp.float32
    ) + jnp.dot(low, returned, preferred_element_type=jnp.float32)
    shared_result = jnp.dot(whole_shared, shared_down_weight, preferred_element_type=jnp.float32)
    routed_out = (routed_sum + shared_result).astype(jnp.bfloat16)
    return (mixer_output, routed_out)


def solution(mesh):
    return jax.shard_map(
        on_device,
        mesh=mesh,
        in_specs=(
            P("ep", "tp"),
            P("ep", "tp"),
            P("ep", "tp"),
            P("ep", "tp"),
            P("ep", "tp"),
            P("ep", "tp"),
            P("tp"),
            P("tp"),
            P(None, "tp"),
            P(None, "tp"),
            P(None, "tp"),
            P("tp"),
            P(None, "tp"),
            P("ep", None),
            P(),
            P("ep", None),
            P("ep", None),
            P("ep", None, "tp"),
            P("ep", None, "tp"),
            P("ep", None, "tp"),
            P(None, "tp"),
            P(None, "tp"),
            P(None, "tp"),
        ),
        out_specs=(P("ep", "tp"), P("ep", "tp")),
        check_vma=False,
    )
```
